1024 devices in a mesh: sp: 64 (over z, core), tp: 16 (over y, x).
Axes of the slice: x: 4, y: 4, z: 32, core: 2. Of those that a mesh axis runs over, the one named last changes fastest.
Arguments:
- decoder_inputs: bfloat16 [8192, 2048], P('sp', 'tp'), may hold values from -300 to 300
- encoder_states: bfloat16 [16384, 2048], P('sp'), may hold values from -6 to 6
- rescale_coefficients: float32 [3, 2048], replicated, may hold values from 0.1 to 1.9
- encoder_rescale: float32 [2, 2048], replicated, may hold values from 0.1 to 1.9
- asking_weights: bfloat16 [2, 2048, 2048], P(None, None, 'tp'), may hold values from -0.125 to 0.125
- lookup_weights: bfloat16 [2, 2048, 256], P(None, None, 'tp'), may hold values from -0.125 to 0.125
- content_weights: bfloat16 [2, 2048, 256], P(None, None, 'tp'), may hold values from -0.125 to 0.125
- merging_weights: bfloat16 [2, 2048, 2048], P(None, None, 'tp'), may hold values from -0.25 to 0.25
- sharpness_factors: float32 [2, 16], replicated, may hold values from 1 to 60
- switching_weights: bfloat16 [2048, 6144], P(None, 'tp'), may hold values from -0.125 to 0.125
- expanding_weights: bfloat16 [2048, 6144], P(None, 'tp'), may hold values from -0.125 to 0.125
- contracting_weights: bfloat16 [6144, 2048], P(None, 'tp'), may hold values from -0.078125 to 0.078125
Outputs:
- updated: bfloat16 [8192, 2048], P('sp', 'tp')
The draws below stay inside these ranges and needn't reach their ends.
All inputs are finite; a program needn't handle non-finite values.
Results may differ from the reference program's by a relative error of at most 0.024.
Values may be sent and summed in bfloat16 or wider, within the bound.
A program may use at most 64 MiB of HBM per device.

```python
import jax
import jax.numpy as jnp
from jax import lax

D = 2048
CHANNEL_WIDTH = 128
QH = 16
SHARED_LOOKUPS = 2
FF = 6144
T_DEV = 128
S_DEV = 256
TGT = 8192
SRC = 16384
N_SP = 64
N_TP = 16


def draw_decoder_inputs(key, part):
    key_base, key_rise = jax.random.split(key, 2)
    normal_part = jax.random.normal(key_base, (TGT, D), jnp.float32)
    column_pos = jnp.arange(D, dtype=jnp.float32) / D
    column_rise = jnp.exp(jnp.log(3.0) * column_pos + 0.3 * jax.random.uniform(key_rise, (D,), jnp.float32))
    return (normal_part * column_rise).astype(jnp.bfloat16)


def draw_sharpness_factors(key, part):
    key_base = jax.random.fold_in(key, 0)
    levels = jnp.exp(jnp.log(4.0) * jax.random.uniform(key_base, (2, QH), jnp.float32))
    return levels


def level_of(own_key, shape, shards, smallest, top_value):
    factor_of, own = 1.0, jax.random.fold_in(own_key, 6)
    for dim, blocks in shards:
        draws = jnp.exp(jax.random.uniform(jax.random.fold_in(own, dim), (blocks,), jnp.float32, smallest / len(shards), top_value / len(shards)))
        factor_of = factor_of * jnp.repeat(draws, shape[dim] // blocks).reshape([-1 if axis == dim else 1 for axis in range(len(shape))])
    return factor_of


def gaussian(own_key, extent, spread, most, pieces=(), held_as=jnp.bfloat16):
    result = jax.random.normal(own_key, extent, jnp.float32) * spread
    if len(pieces) > 0:
        result = level_of(own_key, extent, pieces, -0.22, 0.18) * result
    return jnp.clip(result, min=-most, max=most).astype(held_as)


def setup_inputs(seed: int = 0) -> dict:
    key_list = jax.random.split(jax.random.key(seed), 13)
    return {
        "decoder_inputs": draw_decoder_inputs(jax.random.fold_in(key_list[12], 71), 0),
        "encoder_states": gaussian(key_list[1], (SRC, D), 1.0, 6.0, ((0, 64),)),
        "rescale_coefficients": jnp.clip(1.0 + 0.18 * jax.random.normal(key_list[2], (3, D), jnp.float32), 0.1, 1.9),
        "encoder_rescale": jnp.clip(1.0 + 0.18 * jax.random.normal(key_list[3], (2, D), jnp.float32), 0.1, 1.9),
        "asking_weights": gaussian(key_list[4], (2, D, QH * CHANNEL_WIDTH), D ** -0.5, 0.125, ((2, 16),)),
        "lookup_weights": gaussian(key_list[5], (2, D, SHARED_LOOKUPS * CHANNEL_WIDTH), D ** -0.5, 0.125, ((2, 16),)),
        "content_weights": gaussian(key_list[6], (2, D, SHARED_LOOKUPS * CHANNEL_WIDTH), D ** -0.5, 0.125, ((2, 16),)),
        "merging_weights": gaussian(key_list[7], (2, QH * CHANNEL_WIDTH, D), (QH * CHANNEL_WIDTH // 4) ** -0.5, 0.25, ((2, 16),)),
        "sharpness_factors": draw_sharpness_factors(jax.random.fold_in(key_list[12], 71), 0),
        "switching_weights": gaussian(key_list[9], (D, FF), D ** -0.5, 0.125, ((1, 16),)),
        "expanding_weights": gaussian(key_list[10], (D, FF), D ** -0.5, 0.125, ((1, 16),)),
        "contracting_weights": gaussian(key_list[11], (FF, D), FF ** -0.5, 0.078125, ((1, 16),)),
    }


EPSILON = 1e-06

def normed_product(row_data, gain, weight):
    widened = row_data.astype(jnp.float32)
    scaling = lax.rsqrt(lax.optimization_barrier(jnp.mean(widened * widened, axis=1, keepdims=True)) + EPSILON)
    normed = (widened * gain).astype(jnp.bfloat16)
    return jnp.dot(normed, weight, preferred_element_type=jnp.float32) * scaling

def stored(values):
    return lax.optimization_barrier(values.astype(jnp.bfloat16))

def decoder_encoder_update(asking_entries, encoder_lookups, encoder_contents, sharpness_factors):
    askers_sharing_lookup = QH // SHARED_LOOKUPS
    span_rows = S_DEV // N_TP
    blocks = asking_entries.reshape(N_SP, T_DEV, SHARED_LOOKUPS, askers_sharing_lookup, CHANNEL_WIDTH)
    key_sets = encoder_lookups.reshape(N_SP, N_TP, span_rows, SHARED_LOOKUPS, CHANNEL_WIDTH).transpose(1, 0, 2, 3, 4)
    key_sets = key_sets.reshape(N_TP, N_SP * span_rows, SHARED_LOOKUPS, CHANNEL_WIDTH).astype(jnp.float32)
    value_sets = encoder_contents.reshape(N_SP, N_TP, span_rows, SHARED_LOOKUPS, CHANNEL_WIDTH).transpose(1, 0, 2, 3, 4)
    value_sets = value_sets.reshape(N_TP, N_SP * span_rows, SHARED_LOOKUPS, CHANNEL_WIDTH).astype(jnp.float32)
    softmax_factor = (sharpness_factors * CHANNEL_WIDTH ** (-0.5)).reshape(SHARED_LOOKUPS, askers_sharing_lookup)

    def one_block(query_block):
        widened = query_block.astype(jnp.float32)
        scores = jnp.einsum('tgrd,jkgd->jtgrk', widened, key_sets) * softmax_factor[None, None, :, :, None]
        maxima = lax.optimization_barrier(jnp.max(scores, axis=4))
        expwts = jnp.exp(scores - maxima[..., None])
        totals = lax.optimization_barrier(jnp.sum(expwts, axis=4))
        rounded = lax.optimization_barrier(expwts.astype(jnp.bfloat16)).astype(jnp.float32)
        partials = jnp.einsum('jtgrk,jkgd->jtgrd', rounded, value_sets) / totals[..., None]
        partials = lax.optimization_barrier(partials.astype(jnp.bfloat16)).astype(jnp.float32)
        largest = lax.optimization_barrier(jnp.max(maxima, axis=0))
        mixing = jnp.exp(maxima - largest) * totals
        merged = lax.optimization_barrier(jnp.sum(mixing[..., None] * partials, axis=0)) / lax.optimization_barrier(jnp.sum(mixing, axis=0))[..., None]
        return merged.reshape(T_DEV, QH * CHANNEL_WIDTH).astype(jnp.bfloat16)
    return lax.map(one_block, blocks).reshape(N_SP * T_DEV, QH * CHANNEL_WIDTH)

def reference(decoder_inputs, encoder_states, rescale_coefficients, encoder_rescale, asking_weights, lookup_weights, content_weights, merging_weights, sharpness_factors, switching_weights, expanding_weights, contracting_weights):
    stream = decoder_inputs
    for tier_index in range(2):
        encoder_lookups = stored(normed_product(encoder_states, encoder_rescale[tier_index], lookup_weights[tier_index]))
        encoder_contents = stored(normed_product(encoder_states, encoder_rescale[tier_index], content_weights[tier_index]))
        asking_entries = stored(normed_product(stream, rescale_coefficients[tier_index], asking_weights[tier_index]))
        mixed_entries = decoder_encoder_update(asking_entries, encoder_lookups, encoder_contents, sharpness_factors[tier_index])
        branch = jnp.dot(mixed_entries, merging_weights[tier_index], preferred_element_type=jnp.float32)
        stream = stored(stream.astype(jnp.float32) + branch)
    gate_sum = normed_product(stream, rescale_coefficients[2], switching_weights)
    up_sum = normed_product(stream, rescale_coefficients[2], expanding_weights)
    hidden = stored(jax.nn.silu(gate_sum) * up_sum)
    branch = jnp.dot(hidden, contracting_weights, preferred_element_type=jnp.float32)
    return (stream.astype(jnp.float32) + branch).astype(jnp.bfloat16)
```

```python
import math

import jax
import jax.numpy as jnp
from jax import lax
from jax.experimental import pallas as pl
from jax.experimental.pallas import tpu as pltpu
from jax.sharding import PartitionSpec as P

MESH = pl.DeviceIdType.MESH
D = 2048
HEAD = 128
EPSILON = 1e-06
LOG2E = 1.4426950408889634
F32 = jnp.float32
BF16 = jnp.bfloat16
NZ = 32
X0, X1, X2, A0, A1, H0 = range(6)
C0, Q0, Q1, O0, O1, M0, M1 = range(7)
FULL = [(dy, dx) for dy in range(4) for dx in range(4) if dy or dx]
HALF = [(dy, dx) for dy in range(2) for dx in range(4) if dy or dx]


def slot(d):
    return (d + 1) % NZ


def kernel(
    x_hbm, enc_hbm, gain_ref, egain_ref, wq_hbm, wk_hbm, wv_hbm, wo_hbm, sharp_ref, wg_hbm, wu_hbm, wd_hbm,
    out_ref,
    x_v, enc_v, wkv, wq_v, wo_v, wg_v, wu_v, wd_v,
    comp, rbuf, kvbuf, xbuf, qown, qbuf, osend, mlsend, obuf, mlbuf, aown, abuf, sown, hown, hbuf,
    o_acc, m_acc, l_acc, cvec,
    lsem, psend, precv, hsend, hrecv, zsend_sem, zrecv_sem,
):
    t = lax.axis_index("tp")
    s = lax.axis_index("sp")
    y, x = t // 4, t % 4
    g, r = t // 8, t % 8
    z, c = s // 2, s % 2

    locals_ = {}

    def fetch(i, src, dst):
        cp = pltpu.make_async_copy(src, dst, lsem.at[i])
        cp.start()
        locals_[i] = cp

    fetch(0, enc_hbm, enc_v)
    for l in range(2):
        fetch(1 + 2 * l, wk_hbm.at[l], wkv.at[pl.ds(32 * l, 16)])
        fetch(2 + 2 * l, wv_hbm.at[l], wkv.at[pl.ds(32 * l + 16, 16)])
    fetch(5, x_hbm, x_v)
    fetch(6, wq_hbm, wq_v)
    fetch(7, wo_hbm, wo_v)
    fetch(8, wg_hbm, wg_v)
    fetch(9, wu_hbm, wu_v)
    fetch(10, wd_hbm, wd_v)

    def plane_peer(dy, dx):
        return ((y + dy) % 4) * 4 + (x + dx) % 4

    def half_peer(dy, dx):
        return g * 8 + ((y % 2 + dy) % 2) * 4 + (x + dx) % 4

    def z_peer(dz):
        return ((z + dz + NZ) % NZ) * 2 + c

    partner = z * 2 + (1 - c)
    barrier = pltpu.get_barrier_semaphore()
    for dy, dx in FULL:
        pl.semaphore_signal(barrier, inc=1, device_id={"tp": plane_peer(dy, dx)}, device_id_type=MESH)
    for dz in (-4, -2, -1, 1, 2, 4):
        pl.semaphore_signal(barrier, inc=1, device_id={"sp": z_peer(dz)}, device_id_type=MESH)
    pl.semaphore_signal(barrier, inc=1, device_id={"sp": partner}, device_id_type=MESH)

    pending = []

    def plane_send(e, src, dst):
        for dy, dx in FULL:
            d = dy * 4 + dx
            cp = pltpu.make_async_remote_copy(
                src_ref=src, dst_ref=dst, send_sem=psend.at[e, d], recv_sem=precv.at[e, d],
                device_id={"tp": plane_peer(dy, dx)}, device_id_type=MESH,
            )
            cp.start()
            pending.append(cp)

    def plane_wait(e, dst_of):
        for dy, dx in FULL:
            d = dy * 4 + dx
            source = ((y - dy + 4) % 4) * 4 + (x - dx + 4) % 4
            ref = dst_of(source)
            pltpu.make_async_remote_copy(
                src_ref=ref, dst_ref=ref, send_sem=psend.at[e, d], recv_sem=precv.at[e, d],
                device_id={"tp": source}, device_id_type=MESH,
            ).wait_recv()

    def half_send(e, src_of, dst):
        for dy, dx in HALF:
            d = dy * 4 + dx
            peer = half_peer(dy, dx)
            cp = pltpu.make_async_remote_copy(
                src_ref=src_of(peer % 8), dst_ref=dst, send_sem=hsend.at[e, d], recv_sem=hrecv.at[e, d],
                device_id={"tp": peer}, device_id_type=MESH,
            )
            cp.start()
            pending.append(cp)

    def half_wait(e, dst_of):
        for dy, dx in HALF:
            d = dy * 4 + dx
            source = ((y % 2 - dy + 2) % 2) * 4 + (x - dx + 4) % 4
            ref = dst_of(source)
            pltpu.make_async_remote_copy(
                src_ref=ref, dst_ref=ref, send_sem=hsend.at[e, d], recv_sem=hrecv.at[e, d],
                device_id={"tp": g * 8 + source}, device_id_type=MESH,
            ).wait_recv()

    counts = [0, 0]

    def z_copy(l, d, dz, device):
        k = counts[l]
        counts[l] += 1
        cp = pltpu.make_async_remote_copy(
            src_ref=kvbuf.at[l, slot(d), c], dst_ref=kvbuf.at[l, slot(d - dz), c],
            send_sem=zsend_sem.at[l, k], recv_sem=zrecv_sem.at[l, slot(d - dz) * 2 + c],
            device_id={"sp": device}, device_id_type=MESH,
        )
        cp.start()
        pending.append(cp)

    def z_wait(l, d, cc):
        ref = kvbuf.at[l, slot(d), cc]
        pltpu.make_async_remote_copy(
            src_ref=ref, dst_ref=ref, send_sem=zsend_sem.at[l, 0], recv_sem=zrecv_sem.at[l, slot(d) * 2 + cc],
            device_id={"sp": partner}, device_id_type=MESH,
        ).wait_recv()

    def z_near(l, d):
        z_copy(l, d, 1, z_peer(1))
        z_copy(l, d, -1, z_peer(-1))
        if d in (0, -4, -8, -12):
            z_copy(l, d, 2, z_peer(2))
        if d in (0, 4, 8, 12):
            z_copy(l, d, -2, z_peer(-2))
        z_copy(l, d, 0, partner)

    def z_start(l):
        z_copy(l, 0, 4, z_peer(4))
        z_copy(l, 0, -4, z_peer(-4))
        z_near(l, 0)

    def z_jump(l, k):
        z_wait(l, -4 * k, c)
        if k < 4:
            z_copy(l, -4 * k, 4, z_peer(4))
        z_near(l, -4 * k)
        if k < 4:
            z_wait(l, 4 * k, c)
            if k < 3:
                z_copy(l, 4 * k, -4, z_peer(-4))
            z_near(l, 4 * k)

    def z_neighbours(l, d):
        near = [d - 1, d + 1]
        if d in (0, -4, -8, -12):
            near.append(d - 2)
        if d in (0, 4, 8, 12):
            near.append(d + 2)
        for e in near:
            z_wait(l, e, c)
            z_copy(l, e, 0, partner)

    JUMPS = (0, -4, 4, -8, 8, -12, 12, -16)

    locals_[0].wait()
    for i in range(1, 5):
        locals_[i].wait()
    wkv[pl.ds(64, 64), :] = jnp.zeros((64, D), BF16)
    enc = enc_v[...].astype(F32)
    scale = lax.rsqrt(jnp.mean(enc * enc, axis=1, keepdims=True) + EPSILON)
    products = []
    for l in range(2):
        normed = (enc * egain_ref[pl.ds(l, 1), :]).astype(BF16)
        products.append(
            lax.dot_general(normed, wkv[...], (((1,), (1,)), ((), ())), preferred_element_type=F32)
        )
    lane = lax.broadcasted_iota(jnp.int32, (256, 128), 1)
    comp[...] = (jnp.where(lane < 32, products[0], products[1]) * scale).astype(BF16)
    pl.semaphore_wait(barrier, len(FULL) + 7)
    half_send(C0, lambda p: comp.at[pl.ds(pl.multiple_of(p * 32, 32), 32)], rbuf.at[pl.ds(pl.multiple_of(r * 32, 32), 32)])
    rbuf[pl.ds(pl.multiple_of(r * 32, 32), 32), :] = comp[pl.ds(pl.multiple_of(r * 32, 32), 32), :]

    def columns(ref, who, width):
        return ref.at[:, pl.ds(pl.multiple_of(who * width, width), width)]

    locals_[5].wait()
    plane_send(X0, x_v, columns(xbuf.at[0], t, 128))
    columns(xbuf.at[0], t, 128)[...] = x_v[...]

    half_wait(C0, lambda p: rbuf.at[pl.ds(pl.multiple_of(p * 32, 32), 32)])
    row = lax.broadcasted_iota(jnp.int32, (128, 512), 0)
    col = lax.broadcasted_iota(jnp.int32, (128, 512), 1)
    spread = jnp.where((row // 16 == col // 128) & (row % 16 == col % 16), 1.0, 0.0).astype(BF16)
    wide = jnp.dot(rbuf[...], spread, preferred_element_type=F32)
    row = lax.broadcasted_iota(jnp.int32, (256, 512), 0)
    col = lax.broadcasted_iota(jnp.int32, (256, 512), 1)
    wide = jnp.where(row // 32 == (col % 128) // 16, wide, 0.0)
    chunk = jnp.sum(wide.reshape(8, 32, 512), axis=0).astype(BF16)
    kvbuf[0, slot(0), c] = chunk[:, :256]
    kvbuf[1, slot(0), c] = chunk[:, 256:]
    z_start(0)

    def project(l, e):
        plane_wait(e, lambda p: columns(xbuf.at[l], p, 128))
        stream = xbuf[l].astype(F32)
        factor = lax.rsqrt(jnp.mean(stream * stream, axis=1, keepdims=True) + EPSILON)
        normed = (stream * gain_ref[pl.ds(l, 1), :]).astype(BF16)
        return normed, factor

    def queries(l):
        normed, factor = project(l, (X0, X1)[l])
        qown[l] = (jnp.dot(normed, wq_v[l], preferred_element_type=F32) * factor).astype(BF16)
        half_send((Q0, Q1)[l], lambda p: qown.at[l], qbuf.at[l, r])
        qbuf[l, r] = qown[l]

    def attention(l):
        for h in range(8):
            value = sharp_ref[l, g * 8 + h] * (HEAD**-0.5 * LOG2E)
            cvec[:, pl.ds(h * 128, 128)] = jnp.full((1, 128), value, F32)
        m_acc[...] = jnp.full((1, 1024), -1e30, F32)
        l_acc[...] = jnp.zeros((1, 1024), F32)
        o_acc[...] = jnp.zeros((128, 1024), F32)

        def block(j, carry):
            kv = kvbuf[l, pl.ds(4 * j, 4)].reshape(256, 256)
            q = qbuf[l].reshape(1024, 128)
            scores = lax.dot_general(kv[:, :128], q, (((1,), (1,)), ((), ())), preferred_element_type=F32)
            scores = scores * cvec[...]
            m_old = m_acc[...]
            m_new = jnp.maximum(m_old, jnp.max(scores, axis=0, keepdims=True))
            p = jnp.exp2(scores - m_new)
            shrink = jnp.exp2(m_old - m_new)
            m_acc[...] = m_new
            l_acc[...] = l_acc[...] * shrink + jnp.sum(p, axis=0, keepdims=True)
            o_acc[...] = o_acc[...] * shrink + lax.dot_general(
                kv[:, 128:], p.astype(BF16), (((0,), (0,)), ((), ())), preferred_element_type=F32
            )
            return carry

        lax.fori_loop(0, 8, block, 0)
        for h in range(8):
            at = pl.ds(h * 128, 128)
            osend[l, h] = (o_acc[:, at] / l_acc[:, at]).astype(BF16)
            mlsend[l, h, pl.ds(0, 1), :] = m_acc[:, at]
            mlsend[l, h, pl.ds(1, 7), :] = jnp.broadcast_to(l_acc[:, at], (7, 128))
        half_send((O0, O1)[l], lambda p: osend.at[l, p], obuf.at[l, r])
        half_send((M0, M1)[l], lambda p: mlsend.at[l, p], mlbuf.at[l, r])
        obuf[l, r] = osend[l, r]
        mlbuf[l, r] = mlsend[l, r]

    def merge(l):
        half_wait((O0, O1)[l], lambda p: obuf.at[l, p])
        half_wait((M0, M1)[l], lambda p: mlbuf.at[l, p])
        ml = mlbuf[l]
        maxima, totals = ml[:, 0:1, :], ml[:, 1:2, :]
        mixing = jnp.exp2(maxima - jnp.max(maxima, axis=0, keepdims=True)) * totals
        mixing = mixing / jnp.sum(mixing, axis=0, keepdims=True)
        merged = jnp.sum(obuf[l].astype(F32) * mixing, axis=0)
        aown[l] = merged.T.astype(BF16)
        plane_send((A0, A1)[l], aown.at[l], columns(abuf.at[l], t, 128))
        columns(abuf.at[l], t, 128)[...] = aown[l]

    def output(l, previous):
        plane_wait((A0, A1)[l], lambda p: columns(abuf.at[l], p, 128))
        branch = jnp.dot(abuf[l], wo_v[l], preferred_element_type=F32)
        sown[l] = (previous.astype(F32) + branch).astype(BF16)
        plane_send((X1, X2)[l], sown.at[l], columns(xbuf.at[l + 1], t, 128))
        columns(xbuf.at[l + 1], t, 128)[...] = sown[l]

    z_jump(0, 1)
    locals_[6].wait()
    queries(0)
    for k in (2, 3, 4):
        z_jump(0, k)
    for d in JUMPS:
        z_neighbours(0, d)
    z_start(1)
    for d in range(NZ):
        z_wait(0, d, 1 - c)
    half_wait(Q0, lambda p: qbuf.at[0, p])
    attention(0)
    z_jump(1, 1)
    z_jump(1, 2)
    merge(0)
    z_jump(1, 3)
    z_jump(1, 4)
    locals_[7].wait()
    output(0, x_v[...])
    for d in JUMPS:
        z_neighbours(1, d)
    queries(1)
    for d in range(NZ):
        z_wait(1, d, 1 - c)
    half_wait(Q1, lambda p: qbuf.at[1, p])
    attention(1)
    merge(1)
    output(1, sown[0])

    normed, factor = project(2, X2)
    locals_[8].wait()
    locals_[9].wait()
    gate = jnp.dot(normed, wg_v[...], preferred_element_type=F32) * factor
    up = jnp.dot(normed, wu_v[...], preferred_element_type=F32) * factor
    hown[...] = (gate / (1.0 + jnp.exp(-gate)) * up).astype(BF16)
    plane_send(H0, hown, columns(hbuf, t, 384))
    columns(hbuf, t, 384)[...] = hown[...]
    plane_wait(H0, lambda p: columns(hbuf, p, 384))
    locals_[10].wait()
    branch = jnp.dot(hbuf[...], wd_v[...], preferred_element_type=F32)
    out_ref[...] = (sown[1].astype(F32) + branch).astype(BF16)
    for cp in pending:
        cp.wait_send()


def per_device(x, enc, gains, egains, wq, wk, wv, wo, sharp, wg, wu, wd):
    anywhere = pl.BlockSpec(memory_space=pl.ANY)
    vmem = pl.BlockSpec(memory_space=pltpu.VMEM)
    smem = pl.BlockSpec(memory_space=pltpu.SMEM)
    scratch = [
        pltpu.VMEM((128, 128), BF16),
        pltpu.VMEM((256, D), BF16),
        pltpu.VMEM((128, D), BF16),
        pltpu.VMEM((2, D, 128), BF16),
        pltpu.VMEM((2, D, 128), BF16),
        pltpu.VMEM((D, 384), BF16),
        pltpu.VMEM((D, 384), BF16),
        pltpu.VMEM((6144, 128), BF16),
        pltpu.VMEM((256, 128), BF16),
        pltpu.VMEM((256, 128), BF16),
        pltpu.VMEM((2, NZ, 2, 32, 256), BF16),
        pltpu.VMEM((3, 128, D), BF16),
        pltpu.VMEM((2, 128, 128), BF16),
        pltpu.VMEM((2, 8, 128, 128), BF16),
        pltpu.VMEM((2, 8, 128, 128), BF16),
        pltpu.VMEM((2, 8, 8, 128), F32),
        pltpu.VMEM((2, 8, 128, 128), BF16),
        pltpu.VMEM((2, 8, 8, 128), F32),
        pltpu.VMEM((2, 128, 128), BF16),
        pltpu.VMEM((2, 128, D), BF16),
        pltpu.VMEM((2, 128, 128), BF16),
        pltpu.VMEM((128, 384), BF16),
        pltpu.VMEM((128, 6144), BF16),
        pltpu.VMEM((128, 1024), F32),
        pltpu.VMEM((1, 1024), F32),
        pltpu.VMEM((1, 1024), F32),
        pltpu.VMEM((1, 1024), F32),
        pltpu.SemaphoreType.DMA((11,)),
        pltpu.SemaphoreType.DMA((6, 16)),
        pltpu.SemaphoreType.DMA((6, 16)),
        pltpu.SemaphoreType.DMA((7, 8)),
        pltpu.SemaphoreType.DMA((7, 8)),
        pltpu.SemaphoreType.DMA((2, 64)),
        pltpu.SemaphoreType.DMA((2, 64)),
    ]
    return pl.pallas_call(
        kernel,
        out_shape=jax.ShapeDtypeStruct((128, 128), BF16),
        in_specs=[anywhere, anywhere, vmem, vmem, anywhere, anywhere, anywhere, anywhere, smem] + [anywhere] * 3,
        out_specs=vmem,
        scratch_shapes=scratch,
        compiler_params=pltpu.CompilerParams(
            collective_id=0, has_side_effects=True, vmem_limit_bytes=60 * 1024 * 1024
        ),
        name="decoder",
    )(x, enc, gains, egains, wq, jnp.swapaxes(wk, 1, 2), jnp.swapaxes(wv, 1, 2), wo, sharp, wg, wu, wd)


def solution(mesh):
    placed = (
        P("sp", "tp"),
        P("sp", None),
        P(),
        P(),
        P(None, None, "tp"),
        P(None, None, "tp"),
        P(None, None, "tp"),
        P(None, None, "tp"),
        P(),
        P(None, "tp"),
        P(None, "tp"),
        P(None, "tp"),
    )
    return jax.shard_map(per_device, mesh=mesh, in_specs=placed, out_specs=P("sp", "tp"), check_vma=False)
```
